32 devices in a mesh: sp: 8 (over z, x), tp: 4 (over y, core).
Axes of the slice: x: 2, y: 2, z: 4, core: 2. Of those that a mesh axis runs over, the one named last changes fastest.
Arguments:
- tokens: bfloat16 [1024, 2048], P(('sp', 'tp')), may hold values from -6 to 6
- norm_gain: float32 [2048], replicated, may hold values from 0.1 to 1.9
- w_query: bfloat16 [2048, 512], P(None, 'tp'), may hold values from -0.125 to 0.125
- w_key: bfloat16 [2048, 512], P(None, 'tp'), may hold values from -0.125 to 0.125
- w_value: bfloat16 [2048, 512], P(None, 'tp'), may hold values from -0.125 to 0.125
- score_offset: float32 [8], P('tp'), may hold values from -13 to -3, as said below
- w_out: bfloat16 [512, 2048], P('tp'), may hold values from -0.25 to 0.25
Outputs:
- mixed: bfloat16 [1024, 2048], P(('sp', 'tp'))
The draws below stay inside these ranges and needn't reach their ends.
Inputs may be any that keep to these rules, and one draw needn't show every extreme that they name: `score_offset`: one offset a head.
All inputs are finite; a program needn't handle non-finite values.
Results may differ from the reference program's by a relative error of at most 0.01.
Values may be sent and summed in bfloat16 or wider, within the bound.
A program may use at most 64 MiB of HBM per device.

```python
import math
import jax
import jax.numpy as jnp
from jax import lax

D = 2048
HEADS = 8
HEAD_DIM = 64
SEQ = 1024
WIDTH = 512
N_TP = 4


def draw_score_offset(key, part):
    key_slow, key_fast, key_pick = jax.random.split(jax.random.fold_in(key, 7), 3)
    slow_level = -jnp.log(jnp.float32(SEQ)) + jax.random.uniform(key_slow, (HEADS,), jnp.float32, -0.5, 0.5)
    fast_level = jax.random.uniform(key_fast, (HEADS,), jnp.float32, -4.5, -3.0)
    ranks = jax.random.permutation(key_pick, HEADS)
    slow_heads = ranks < HEADS // 2
    return jnp.where(slow_heads, slow_level, fast_level).astype(jnp.float32)


def shard_levels(key, extent, cuts, smallest, high):
    gain, own = 1.0, jax.random.fold_in(key, 6)
    for position, parts in cuts:
        steps = jnp.exp(jax.random.uniform(jax.random.fold_in(own, position), (parts,), jnp.float32, smallest / len(cuts), high / len(cuts)))
        gain = gain * jnp.repeat(steps, extent[position] // parts).reshape([-1 if axis == position else 1 for axis in range(len(extent))])
    return gain


def centred(rng, extent, spread, bound, pieces=(), kind=jnp.bfloat16):
    result = spread * jax.random.normal(rng, extent, jnp.float32)
    if pieces:
        result = result * shard_levels(rng, extent, pieces, -0.22, 0.18)
    return jnp.clip(result, -bound, bound).astype(kind)


def setup_inputs(seed: int = 0) -> dict:
    key_of = jax.random.split(jax.random.key(seed), 8)
    return {
        "tokens": centred(key_of[0], (SEQ, D), 1.0, 6.0, ((0, 32),)),
        "norm_gain": jnp.clip(1.0 + 0.18 * jax.random.normal(key_of[1], (D,), jnp.float32), 0.1, 1.9),
        "w_query": centred(key_of[2], (D, WIDTH), D ** -0.5, 0.125, ((1, 4),)),
        "w_key": centred(key_of[3], (D, WIDTH), D ** -0.5, 0.125, ((1, 4),)),
        "w_value": centred(key_of[4], (D, WIDTH), D ** -0.5, 0.125, ((1, 4),)),
        "score_offset": draw_score_offset(jax.random.fold_in(key_of[7], 71), 0),
        "w_out": centred(key_of[6], (WIDTH, D), WIDTH ** -0.5, 0.25, ((0, 4),)),
    }


RMS_EPS = 1e-06

def reference(tokens, norm_gain, w_query, w_key, w_value, score_offset, w_out):
    rows_f32 = tokens.astype(jnp.float32)
    inv_rms = lax.rsqrt(lax.optimization_barrier(jnp.mean(rows_f32 * rows_f32, axis=1, keepdims=True)) + RMS_EPS)
    normed = (rows_f32 * inv_rms * norm_gain.astype(jnp.float32)).astype(jnp.bfloat16)
    queries = jnp.dot(normed, w_query, preferred_element_type=jnp.float32).astype(jnp.bfloat16)
    keys = jnp.dot(normed, w_key, preferred_element_type=jnp.float32).astype(jnp.bfloat16)
    values = jnp.dot(normed, w_value, preferred_element_type=jnp.float32).astype(jnp.bfloat16)
    query_heads = queries.reshape(SEQ, HEADS, HEAD_DIM).transpose(1, 0, 2)
    key_heads = keys.reshape(SEQ, HEADS, HEAD_DIM).transpose(1, 0, 2)
    value_heads = values.reshape(SEQ, HEADS, HEAD_DIM).transpose(1, 0, 2)
    block_rows = math.gcd(SEQ, 512)
    blocks = SEQ // block_rows
    key_pos = jnp.arange(SEQ, dtype=jnp.int32)

    def head_fn(args):
        query_part, key_part, value_part, offset = args

        def block_fn(index):
            start = (index * block_rows).astype(jnp.int32)
            query_rows = lax.dynamic_slice_in_dim(query_part, start, block_rows, 0)
            scores = jnp.dot(query_rows, key_part.T, preferred_element_type=jnp.float32) * HEAD_DIM ** (-0.5) + offset
            query_pos = start + jnp.arange(block_rows, dtype=jnp.int32)
            earlier = key_pos[None, :] < query_pos[:, None]
            log_keep = jnp.where(earlier, jax.nn.log_sigmoid(-scores), 0.0)
            suffix = lax.cumsum(log_keep, axis=1, reverse=True) - log_keep
            weights = jnp.where(earlier, jnp.exp(jax.nn.log_sigmoid(scores) + suffix), 0.0).astype(jnp.bfloat16)
            return jnp.dot(weights, value_part, preferred_element_type=jnp.float32).astype(jnp.bfloat16)
        return lax.map(block_fn, jnp.arange(blocks, dtype=jnp.int32)).reshape(SEQ, HEAD_DIM)
    attended = lax.map(head_fn, (query_heads, key_heads, value_heads, score_offset.astype(jnp.float32)))
    group = HEADS // N_TP
    grouped = attended.reshape(N_TP, group, SEQ, HEAD_DIM).transpose(0, 2, 1, 3).reshape(N_TP, SEQ, group * HEAD_DIM)
    weight_groups = w_out.reshape(N_TP, group * HEAD_DIM, D)

    def partial_fn(args):
        rows, weight = args
        rounded = jnp.dot(rows, weight, preferred_element_type=jnp.float32).astype(jnp.bfloat16)
        return lax.optimization_barrier(rounded).astype(jnp.float32)
    partials = lax.map(partial_fn, (grouped, weight_groups))
    return lax.optimization_barrier(jnp.sum(partials, axis=0)).astype(jnp.bfloat16)
```

```python
import functools

import jax
import jax.numpy as jnp
from jax import lax
from jax.experimental import pallas as pl
from jax.experimental.pallas import tpu as pltpu
from jax.sharding import PartitionSpec as P

HEAD_DIM = 64
RMS_EPS = 1e-06
MESH = pl.DeviceIdType.MESH
F32 = jnp.float32
BF16 = jnp.bfloat16


def layer_kernel(
    n_sp,
    n_tp,
    lanes,
    tok_ref,
    gain_ref,
    wq_ref,
    wk_ref,
    wv_ref,
    off_ref,
    wout_ref,
    out_ref,
    tok_buf,
    w_buf,
    wo_buf,
    normed,
    kv_out,
    q_out,
    kv_buf,
    q_buf,
    att_out,
    att_buf,
    load_sem,
    tok_send,
    tok_recv,
    wo_send,
    wo_recv,
    kv_send,
    kv_recv,
    q_send,
    q_recv,
    att_send,
    att_recv,
):
    s = lax.axis_index("sp")
    t = lax.axis_index("tp")
    heads = kv_out.shape[0]
    rows = kv_out.shape[1]
    piece = tok_buf.shape[1]
    width = 2 * HEAD_DIM
    groups = n_sp // heads
    a = s // heads
    b = s % heads
    pair_hi = t // lanes
    pair_lo = t % lanes
    n_hi = n_tp // lanes

    loads = [
        pltpu.make_async_copy(tok_ref, tok_buf.at[t], load_sem.at[0]),
        pltpu.make_async_copy(wq_ref, w_buf.at[:, pl.ds(0, width)], load_sem.at[1]),
        pltpu.make_async_copy(wk_ref, w_buf.at[:, pl.ds(width, width)], load_sem.at[2]),
        pltpu.make_async_copy(wv_ref, w_buf.at[:, pl.ds(2 * width, width)], load_sem.at[3]),
        pltpu.make_async_copy(wout_ref, wo_buf.at[t], load_sem.at[4]),
    ]
    for load in loads:
        load.start()

    barrier = pltpu.get_barrier_semaphore()
    for i in range(1, n_tp):
        other = (t + i) % n_tp
        for j in range(heads):
            peer = a * heads + (b + j) % heads
            pl.semaphore_signal(barrier, inc=1, device_id=(peer, other), device_id_type=MESH)

    def greet(i, carry):
        pl.semaphore_signal(barrier, inc=1, device_id=((s + i) % n_sp, t), device_id_type=MESH)
        return carry

    lax.fori_loop(1, n_sp, greet, 0)
    pl.semaphore_wait(barrier, (n_tp - 1) * heads + n_sp - 1)

    def send(src, dst, send_sem, recv_sem, device):
        return pltpu.make_async_remote_copy(
            src_ref=src,
            dst_ref=dst,
            send_sem=send_sem,
            recv_sem=recv_sem,
            device_id=device,
            device_id_type=MESH,
        )

    def gather(buf, send_sems, recv_sems):
        sends = []
        for i in range(1, n_hi):
            dest = (pair_hi + i) % n_hi * lanes + pair_lo
            sends.append(send(buf.at[t], buf.at[t], send_sems.at[i * lanes], recv_sems.at[t], (s, dest)))
        for j in range(1, lanes):
            dest = pair_hi * lanes + (pair_lo + j) % lanes
            sends.append(send(buf.at[t], buf.at[t], send_sems.at[j], recv_sems.at[t], (s, dest)))
        return sends

    def arrival(buf, recv_sems, source):
        pltpu.make_async_copy(buf.at[source], buf.at[source], recv_sems.at[source]).wait()

    def relays(buf, send_sems, recv_sems, i, source):
        out = []
        for j in range(1, lanes):
            dest = pair_hi * lanes + (pair_lo + j) % lanes
            out.append(
                send(buf.at[source], buf.at[source], send_sems.at[i * lanes + j], recv_sems.at[source], (s, dest))
            )
        return out

    gain = gain_ref[...]

    def norm(source):
        x = tok_buf[source].astype(F32)
        inv = lax.rsqrt(jnp.mean(x * x, axis=1, keepdims=True) + RMS_EPS)
        normed[pl.ds(pl.multiple_of(source * piece, piece), piece), :] = (x * inv * gain).astype(BF16)

    loads[0].wait()
    pending = gather(tok_buf, tok_send, tok_recv)
    for copy in pending:
        copy.start()
    norm(t)
    for j in range(1, lanes):
        source = pair_hi * lanes + (pair_lo + j) % lanes
        arrival(tok_buf, tok_recv, source)
        norm(source)
    for i in range(1, n_hi):
        source = (pair_hi + i) % n_hi * lanes + pair_lo
        arrival(tok_buf, tok_recv, source)
        for copy in relays(tok_buf, tok_send, tok_recv, i, source):
            copy.start()
            pending.append(copy)
        norm(source)
    loads[4].wait()
    wo_pending = gather(wo_buf, wo_send, wo_recv)
    for copy in wo_pending:
        copy.start()
    for i in range(1, n_hi):
        for j in range(1, lanes):
            source = (pair_hi + i) % n_hi * lanes + (pair_lo + j) % lanes
            arrival(tok_buf, tok_recv, source)
            norm(source)
    for load in loads[1:4]:
        load.wait()

    projected = jnp.dot(normed[...], w_buf[...], preferred_element_type=F32).astype(BF16)
    blank = jnp.zeros((rows, HEAD_DIM), BF16)
    for h in range(heads):
        cols = slice(h * HEAD_DIM, (h + 1) * HEAD_DIM)
        keys = projected[:, width:][:, cols]
        vals = projected[:, 2 * width :][:, cols]
        kv_out[h] = jnp.concatenate([keys, vals], axis=1)
        q_out[h] = jnp.concatenate([projected[:, cols] * jnp.asarray(HEAD_DIM**-0.5, BF16), blank], axis=1)

    mine = pl.ds(pl.multiple_of(b * rows, rows), rows)
    kv_sends = []
    for j in range(1, heads):
        h = (b + j) % heads
        dest = (a * heads + h, t)
        kv_sends.append(send(q_out.at[h], q_buf.at[mine], q_send.at[j], q_recv.at[b], dest))
        kv_sends.append(send(kv_out.at[h], kv_buf.at[a, mine], kv_send.at[0, j], kv_recv.at[s], dest))
    for copy in kv_sends:
        copy.start()

    def kv_copy(k, j):
        h = (b + j) % heads
        return send(kv_out.at[h], kv_buf.at[a, mine], kv_send.at[k, j], kv_recv.at[s], ((a + k) * heads + h, t))

    later = groups - 1 - a

    def kv_start(i, carry):
        for j in range(heads):
            kv_copy(later - i, j).start()
        return carry

    lax.fori_loop(0, later, kv_start, 0)
    kv_buf[a, mine, :] = kv_out[b]
    q_buf[mine, :] = q_out[b]

    for j in range(1, heads):
        peer = (b + j) % heads
        spot = pl.ds(pl.multiple_of(peer * rows, rows), rows)
        pltpu.make_async_copy(q_buf.at[spot], q_buf.at[spot], q_recv.at[peer]).wait()

    span = heads * rows
    offset = off_ref[b]
    row_id = lax.broadcasted_iota(jnp.int32, (span, span), 0)
    col_id = lax.broadcasted_iota(jnp.int32, (span, span), 1)
    below = row_id > col_id
    tri = jnp.where(below, 1.0, 0.0).astype(BF16)
    queries = q_buf[...]

    def block(group, masked, total, kept):
        kv = kv_buf[group]
        z = lax.dot_general(queries, kv, (((1,), (1,)), ((), ())), preferred_element_type=F32) + offset
        log_keep = -(jnp.maximum(z, 0.0) + jnp.log1p(jnp.exp(-jnp.abs(z))))
        log_take = z + log_keep
        if masked:
            log_keep = jnp.where(below, log_keep, 0.0)
        high = log_keep.astype(BF16)
        low = (log_keep - high.astype(F32)).astype(BF16)
        suffix = jnp.dot(high, tri, preferred_element_type=F32) + jnp.dot(low, tri, preferred_element_type=F32)
        weights = jnp.exp(log_take + suffix + kept)
        if masked:
            weights = jnp.where(below, weights, 0.0)
        total = total + jnp.dot(weights.astype(BF16), kv, preferred_element_type=F32)
        return total, kept + suffix[:, :1] + log_keep[:, :1]

    def kv_arrival(group, peer):
        spot = kv_buf.at[group, pl.ds(pl.multiple_of(peer * rows, rows), rows)]
        pltpu.make_async_copy(spot, spot, kv_recv.at[group * heads + peer]).wait()

    for j in range(1, heads):
        kv_arrival(a, (b + j) % heads)
    total, kept = block(a, True, jnp.zeros((span, width), F32), jnp.zeros((span, 1), F32))

    def absorb(i, carry):
        group = a - 1 - i
        for peer in range(heads):
            kv_arrival(group, peer)
        return block(group, False, *carry)

    total, kept = lax.fori_loop(0, a, absorb, (total, kept))

    att_out[...] = total.astype(BF16).reshape(att_out.shape)
    att_sends = []
    for j in range(heads):
        for i in range(n_tp):
            if i == 0 and j == 0:
                continue
            peer = (b + j) % heads
            other = (t + i) % n_tp
            att_sends.append(
                send(
                    att_out.at[peer * n_tp + other],
                    att_buf.at[t * heads + b],
                    att_send.at[j * n_tp + i],
                    att_recv.at[t * heads + b],
                    (a * heads + peer, other),
                )
            )
    for copy in att_sends:
        copy.start()
    att_buf[t * heads + b] = att_out[b * n_tp + t]

    for i in range(1, n_hi):
        source = (pair_hi + i) % n_hi * lanes + pair_lo
        arrival(wo_buf, wo_recv, source)
        for copy in relays(wo_buf, wo_send, wo_recv, i, source):
            copy.start()
            wo_pending.append(copy)
    for j in range(heads):
        for i in range(n_tp):
            if i or j:
                arrival(att_buf, att_recv, (t + i) % n_tp * heads + (b + j) % heads)

    def partial(source):
        parts = [att_buf[source * heads + h][:, HEAD_DIM:] for h in range(heads)]
        part = jnp.dot(jnp.concatenate(parts, axis=1), wo_buf[source], preferred_element_type=F32)
        return part.astype(BF16).astype(F32)

    mixed = partial(t)
    for j in range(1, lanes):
        source = pair_hi * lanes + (pair_lo + j) % lanes
        arrival(wo_buf, wo_recv, source)
        mixed = mixed + partial(source)
    for i in range(1, n_hi):
        mixed = mixed + partial((pair_hi + i) % n_hi * lanes + pair_lo)
    for i in range(1, n_hi):
        for j in range(1, lanes):
            source = (pair_hi + i) % n_hi * lanes + (pair_lo + j) % lanes
            arrival(wo_buf, wo_recv, source)
            mixed = mixed + partial(source)
    out_ref[...] = mixed.astype(BF16)

    for copy in pending + wo_pending + kv_sends + att_sends:
        copy.wait_send()

    def kv_done(i, carry):
        for j in range(heads):
            kv_copy(later - i, j).wait_send()
        return carry

    lax.fori_loop(0, later, kv_done, 0)


def per_device(tokens, norm_gain, w_query, w_key, w_value, score_offset, w_out):
    n_tp = lax.axis_size("tp")
    n_sp = lax.axis_size("sp")
    piece, model = tokens.shape
    width = w_query.shape[1]
    heads = score_offset.shape[0]
    rows = piece * n_tp
    lanes = 2 if n_tp % 2 == 0 else 1
    groups = n_sp // heads
    lane_width = 2 * HEAD_DIM
    dma = pltpu.SemaphoreType.DMA
    anywhere = pl.BlockSpec(memory_space=pl.ANY)
    vmem = pl.BlockSpec(memory_space=pltpu.VMEM)
    return pl.pallas_call(
        functools.partial(layer_kernel, n_sp, n_tp, lanes),
        out_shape=jax.ShapeDtypeStruct((piece, w_out.shape[1]), BF16),
        in_specs=[
            anywhere,
            vmem,
            anywhere,
            anywhere,
            anywhere,
            pl.BlockSpec(memory_space=pltpu.SMEM),
            anywhere,
        ],
        out_specs=vmem,
        scratch_shapes=[
            pltpu.VMEM((n_tp, piece, model), BF16),
            pltpu.VMEM((model, 3 * width), BF16),
            pltpu.VMEM((n_tp, width, w_out.shape[1]), BF16),
            pltpu.VMEM((rows, model), BF16),
            pltpu.VMEM((heads, rows, lane_width), BF16),
            pltpu.VMEM((heads, rows, lane_width), BF16),
            pltpu.VMEM((groups, heads * rows, lane_width), BF16),
            pltpu.VMEM((heads * rows, lane_width), BF16),
            pltpu.VMEM((heads * n_tp, piece, lane_width), BF16),
            pltpu.VMEM((heads * n_tp, piece, lane_width), BF16),
            dma((5,)),
            dma((n_tp,)),
            dma((n_tp,)),
            dma((n_tp,)),
            dma((n_tp,)),
            dma((groups, heads)),
            dma((n_sp,)),
            dma((heads,)),
            dma((heads,)),
            dma((heads * n_tp,)),
            dma((heads * n_tp,)),
        ],
        compiler_params=pltpu.CompilerParams(collective_id=0, has_side_effects=True),
    )(tokens, norm_gain.reshape(1, model), w_query, w_key, w_value, score_offset, w_out)


def solution(mesh):
    return jax.shard_map(
        per_device,
        mesh=mesh,
        in_specs=(
            P(("sp", "tp"), None),
            P(),
            P(None, "tp"),
            P(None, "tp"),
            P(None, "tp"),
            P("tp"),
            P("tp", None),
        ),
        out_specs=P(("sp", "tp"), None),
        check_vma=False,
    )
```

```python
import functools

import jax
import jax.numpy as jnp
from jax import lax
from jax.experimental import pallas as pl
from jax.experimental.pallas import tpu as pltpu
from jax.sharding import PartitionSpec as P

HEAD_DIM = 64
RMS_EPS = 1e-06
MESH = pl.DeviceIdType.MESH
F32 = jnp.float32
BF16 = jnp.bfloat16
PIECES = 4


def layer_kernel(
    n_sp,
    n_tp,
    lanes,
    tok_ref,
    gain_ref,
    wq_ref,
    wk_ref,
    wv_ref,
    off_ref,
    wout_ref,
    out_ref,
    tok_buf,
    w_buf,
    wo_buf,
    normed,
    kv_out,
    q_out,
    kv_buf,
    q_buf,
    att_out,
    att_buf,
    chain_sem,
    pair_sem,
    load_sem,
    tok_send,
    tok_recv,
    wo_send,
    wo_recv,
    kv_send,
    kv_recv,
    q_send,
    q_recv,
    att_send,
    att_recv,
):
    s = lax.axis_index("sp")
    t = lax.axis_index("tp")
    heads = kv_out.shape[0]
    rows = kv_out.shape[1]
    piece = tok_buf.shape[1]
    width = 2 * HEAD_DIM
    groups = n_sp // heads
    a = s // heads
    b = s % heads
    pair_hi = t // lanes
    pair_lo = t % lanes
    n_hi = n_tp // lanes

    loads = [
        pltpu.make_async_copy(tok_ref, tok_buf.at[t], load_sem.at[0]),
        pltpu.make_async_copy(wq_ref, w_buf.at[:, pl.ds(0, width)], load_sem.at[1]),
        pltpu.make_async_copy(wk_ref, w_buf.at[:, pl.ds(width, width)], load_sem.at[2]),
        pltpu.make_async_copy(wv_ref, w_buf.at[:, pl.ds(2 * width, width)], load_sem.at[3]),
        pltpu.make_async_copy(wout_ref, wo_buf.at[t], load_sem.at[4]),
    ]
    for load in loads:
        load.start()

    barrier = pltpu.get_barrier_semaphore()
    for i in range(1, n_tp):
        pl.semaphore_signal(barrier, inc=1, device_id=(s, (t + i) % n_tp), device_id_type=MESH)
    for j in range(1, heads):
        pl.semaphore_signal(barrier, inc=1, device_id=(a * heads + (b + j) % heads, t), device_id_type=MESH)
    has_next = a < groups - 1
    has_prev = a > 0

    @pl.when(has_next)
    def _():
        pl.semaphore_signal(barrier, inc=1, device_id=(s + heads, t), device_id_type=MESH)

    @pl.when(has_prev)
    def _():
        pl.semaphore_signal(barrier, inc=1, device_id=(s - heads, t), device_id_type=MESH)

    along = jnp.minimum(a, 1) + jnp.minimum(groups - 1 - a, 1)
    pl.semaphore_wait(barrier, n_tp - 1 + heads - 1 + along)

    def send(src, dst, send_sem, recv_sem, device):
        return pltpu.make_async_remote_copy(
            src_ref=src,
            dst_ref=dst,
            send_sem=send_sem,
            recv_sem=recv_sem,
            device_id=device,
            device_id_type=MESH,
        )

    def gather(buf, send_sems, recv_sems):
        sends = []
        for i in range(1, n_hi):
            dest = (pair_hi + i) % n_hi * lanes + pair_lo
            sends.append(send(buf.at[t], buf.at[t], send_sems.at[i * lanes], recv_sems.at[t], (s, dest)))
        for j in range(1, lanes):
            dest = pair_hi * lanes + (pair_lo + j) % lanes
            sends.append(send(buf.at[t], buf.at[t], send_sems.at[j], recv_sems.at[t], (s, dest)))
        return sends

    def arrival(buf, recv_sems, source):
        pltpu.make_async_copy(buf.at[source], buf.at[source], recv_sems.at[source]).wait()

    def relays(buf, send_sems, recv_sems, i, source):
        out = []
        for j in range(1, lanes):
            dest = pair_hi * lanes + (pair_lo + j) % lanes
            out.append(
                send(buf.at[source], buf.at[source], send_sems.at[i * lanes + j], recv_sems.at[source], (s, dest))
            )
        return out

    wo_rows = wo_buf.shape[1] // PIECES

    class wo_piece:
        def __init__(self, c):
            self.rows = pl.ds(c * wo_rows, wo_rows)

        @property
        def at(self):
            return self

        def __getitem__(self, source):
            return wo_buf.at[source, self.rows]

    def wo_relay(c):
        for i in range(1, n_hi):
            source = (pair_hi + i) % n_hi * lanes + pair_lo
            arrival(wo_piece(c), wo_recv.at[c], source)
            for copy in relays(wo_piece(c), wo_send.at[c], wo_recv.at[c], i, source):
                copy.start()
                wo_pending.append(copy)

    def wo_arrival(source):
        for c in range(PIECES):
            arrival(wo_piece(c), wo_recv.at[c], source)

    gain = gain_ref[...]

    def norm(source):
        x = tok_buf[source].astype(F32)
        inv = lax.rsqrt(jnp.mean(x * x, axis=1, keepdims=True) + RMS_EPS)
        normed[pl.ds(pl.multiple_of(source * piece, piece), piece), :] = (x * inv * gain).astype(BF16)

    loads[0].wait()
    pending = gather(tok_buf, tok_send, tok_recv)
    for copy in pending:
        copy.start()

    loads[4].wait()
    wo_pending = []
    for c in range(PIECES):
        for copy in gather(wo_piece(c), wo_send.at[c], wo_recv.at[c]):
            copy.start()
            wo_pending.append(copy)

    @pl.when(has_next)
    def _():
        pl.semaphore_wait(chain_sem, 1)

    @pl.when(has_prev)
    def _():
        pl.semaphore_signal(chain_sem, inc=1, device_id=(s - heads, t), device_id_type=MESH)

    for j in range(1, heads):
        pl.semaphore_signal(pair_sem, inc=1, device_id=(a * heads + (b + j) % heads, t), device_id_type=MESH)
    norm(t)
    for j in range(1, lanes):
        source = pair_hi * lanes + (pair_lo + j) % lanes
        arrival(tok_buf, tok_recv, source)
        norm(source)
    for i in range(1, n_hi):
        source = (pair_hi + i) % n_hi * lanes + pair_lo
        arrival(tok_buf, tok_recv, source)
        for copy in relays(tok_buf, tok_send, tok_recv, i, source):
            copy.start()
            pending.append(copy)
        norm(source)
    pl.semaphore_wait(pair_sem, heads - 1)
    for i in range(1, n_hi):
        for j in range(1, lanes):
            source = (pair_hi + i) % n_hi * lanes + (pair_lo + j) % lanes
            arrival(tok_buf, tok_recv, source)
            norm(source)
    for load in loads[1:4]:
        load.wait()

    projected = jnp.dot(normed[...], w_buf[...], preferred_element_type=F32).astype(BF16)
    blank = jnp.zeros((rows, HEAD_DIM), BF16)
    for h in range(heads):
        cols = slice(h * HEAD_DIM, (h + 1) * HEAD_DIM)
        keys = projected[:, width:][:, cols]
        vals = projected[:, 2 * width :][:, cols]
        kv_out[h] = jnp.concatenate([keys, vals], axis=1)
        q_out[h] = jnp.concatenate([projected[:, cols] * jnp.asarray(HEAD_DIM**-0.5, BF16), blank], axis=1)

    mine = pl.ds(pl.multiple_of(b * rows, rows), rows)
    kv_sends = []
    for j in range(1, heads):
        h = (b + j) % heads
        dest = (a * heads + h, t)
        kv_sends.append(send(q_out.at[h], q_buf.at[mine], q_send.at[j], q_recv.at[b], dest))
        kv_sends.append(send(kv_out.at[h], kv_buf.at[a, mine], kv_send.at[0, j], kv_recv.at[s], dest))
    for copy in kv_sends:
        copy.start()

    def kv_copy(k, j):
        h = (b + j) % heads
        return send(kv_out.at[h], kv_buf.at[a, mine], kv_send.at[k, j], kv_recv.at[s], ((a + k) * heads + h, t))

    later = groups - 1 - a

    def kv_start(i, carry):
        for j in range(heads):
            kv_copy(later - i, j).start()
        return carry

    lax.fori_loop(0, later, kv_start, 0)
    kv_buf[a, mine, :] = kv_out[b]
    q_buf[mine, :] = q_out[b]

    for j in range(1, heads):
        peer = (b + j) % heads
        spot = pl.ds(pl.multiple_of(peer * rows, rows), rows)
        pltpu.make_async_copy(q_buf.at[spot], q_buf.at[spot], q_recv.at[peer]).wait()

    span = heads * rows
    offset = off_ref[b]
    row_id = lax.broadcasted_iota(jnp.int32, (span, span), 0)
    col_id = lax.broadcasted_iota(jnp.int32, (span, span), 1)
    below = row_id > col_id
    tri = jnp.where(below, 1.0, 0.0).astype(BF16)
    queries = q_buf[...]

    def block(group, masked, total, kept):
        kv = kv_buf[group]
        z = lax.dot_general(queries, kv, (((1,), (1,)), ((), ())), preferred_element_type=F32) + offset
        log_keep = -(jnp.maximum(z, 0.0) + jnp.log1p(jnp.exp(-jnp.abs(z))))
        log_take = z + log_keep
        if masked:
            log_keep = jnp.where(below, log_keep, 0.0)
        high = log_keep.astype(BF16)
        low = (log_keep - high.astype(F32)).astype(BF16)
        suffix = jnp.dot(high, tri, preferred_element_type=F32) + jnp.dot(low, tri, preferred_element_type=F32)
        weights = jnp.exp(log_take + suffix + kept)
        if masked:
            weights = jnp.where(below, weights, 0.0)
        total = total + jnp.dot(weights.astype(BF16), kv, preferred_element_type=F32)
        return total, kept + suffix[:, :1] + log_keep[:, :1]

    def kv_arrival(group, peer):
        spot = kv_buf.at[group, pl.ds(pl.multiple_of(peer * rows, rows), rows)]
        pltpu.make_async_copy(spot, spot, kv_recv.at[group * heads + peer]).wait()

    for j in range(1, heads):
        kv_arrival(a, (b + j) % heads)
    total, kept = block(a, True, jnp.zeros((span, width), F32), jnp.zeros((span, 1), F32))

    wo_relay(0)

    def absorb(i, carry):
        group = a - 1 - i
        for peer in range(heads):
            kv_arrival(group, peer)
        return block(group, False, *carry)

    total, kept = lax.fori_loop(0, a, absorb, (total, kept))

    att_out[...] = total.astype(BF16).reshape(att_out.shape)
    att_sends = []
    for j in range(heads):
        for i in range(n_tp):
            if i == 0 and j == 0:
                continue
            peer = (b + j) % heads
            other = (t + i) % n_tp
            att_sends.append(
                send(
                    att_out.at[peer * n_tp + other],
                    att_buf.at[t * heads + b],
                    att_send.at[j * n_tp + i],
                    att_recv.at[t * heads + b],
                    (a * heads + peer, other),
                )
            )
    for copy in att_sends:
        copy.start()
    att_buf[t * heads + b] = att_out[b * n_tp + t]

    wo_relay(1)
    wo_relay(2)
    for j in range(heads):
        for i in range(n_tp):
            if i or j:
                arrival(att_buf, att_recv, (t + i) % n_tp * heads + (b + j) % heads)

    def partial(source):
        parts = [att_buf[source * heads + h][:, HEAD_DIM:] for h in range(heads)]
        part = jnp.dot(jnp.concatenate(parts, axis=1), wo_buf[source], preferred_element_type=F32)
        return part.astype(BF16).astype(F32)

    mixed = partial(t)
    for j in range(1, lanes):
        source = pair_hi * lanes + (pair_lo + j) % lanes
        wo_arrival(source)
        mixed = mixed + partial(source)
    for c in range(3, PIECES):
        wo_relay(c)
    for i in range(1, n_hi):
        mixed = mixed + partial((pair_hi + i) % n_hi * lanes + pair_lo)
    for i in range(1, n_hi):
        for j in range(1, lanes):
            source = (pair_hi + i) % n_hi * lanes + (pair_lo + j) % lanes
            wo_arrival(source)
            mixed = mixed + partial(source)
    out_ref[...] = mixed.astype(BF16)

    for copy in pending + wo_pending + kv_sends + att_sends:
        copy.wait_send()

    def kv_done(i, carry):
        for j in range(heads):
            kv_copy(later - i, j).wait_send()
        return carry

    lax.fori_loop(0, later, kv_done, 0)


def per_device(tokens, norm_gain, w_query, w_key, w_value, score_offset, w_out):
    n_tp = lax.axis_size("tp")
    n_sp = lax.axis_size("sp")
    piece, model = tokens.shape
    width = w_query.shape[1]
    heads = score_offset.shape[0]
    rows = piece * n_tp
    lanes = 2 if n_tp % 2 == 0 else 1
    groups = n_sp // heads
    lane_width = 2 * HEAD_DIM
    dma = pltpu.SemaphoreType.DMA
    anywhere = pl.BlockSpec(memory_space=pl.ANY)
    vmem = pl.BlockSpec(memory_space=pltpu.VMEM)
    return pl.pallas_call(
        functools.partial(layer_kernel, n_sp, n_tp, lanes),
        out_shape=pltpu.VMEM((piece, w_out.shape[1]), BF16),
        in_specs=[
            anywhere,
            vmem,
            anywhere,
            anywhere,
            anywhere,
            pl.BlockSpec(memory_space=pltpu.SMEM),
            anywhere,
        ],
        out_specs=vmem,
        scratch_shapes=[
            pltpu.VMEM((n_tp, piece, model), BF16),
            pltpu.VMEM((model, 3 * width), BF16),
            pltpu.VMEM((n_tp, width, w_out.shape[1]), BF16),
            pltpu.VMEM((rows, model), BF16),
            pltpu.VMEM((heads, rows, lane_width), BF16),
            pltpu.VMEM((heads, rows, lane_width), BF16),
            pltpu.VMEM((groups, heads * rows, lane_width), BF16),
            pltpu.VMEM((heads * rows, lane_width), BF16),
            pltpu.VMEM((heads * n_tp, piece, lane_width), BF16),
            pltpu.VMEM((heads * n_tp, piece, lane_width), BF16),
            pltpu.SemaphoreType.REGULAR,
            pltpu.SemaphoreType.REGULAR,
            dma((5,)),
            dma((n_tp,)),
            dma((n_tp,)),
            dma((PIECES, n_tp)),
            dma((PIECES, n_tp)),
            dma((groups, heads)),
            dma((n_sp,)),
            dma((heads,)),
            dma((heads,)),
            dma((heads * n_tp,)),
            dma((heads * n_tp,)),
        ],
        compiler_params=pltpu.CompilerParams(collective_id=0, has_side_effects=True),
    )(tokens, norm_gain.reshape(1, model), w_query, w_key, w_value, score_offset, w_out)


def solution(mesh):
    return jax.shard_map(
        per_device,
        mesh=mesh,
        in_specs=(
            P(("sp", "tp"), None),
            P(),
            P(None, "tp"),
            P(None, "tp"),
            P(None, "tp"),
            P("tp"),
            P("tp", None),
        ),
        out_specs=P(("sp", "tp"), None),
        check_vma=False,
    )
```

```python
import functools

import jax
import jax.numpy as jnp
from jax import lax
from jax.experimental import pallas as pl
from jax.experimental.pallas import tpu as pltpu
from jax.sharding import PartitionSpec as P

HEAD_DIM = 64
RMS_EPS = 1e-06
MESH = pl.DeviceIdType.MESH
F32 = jnp.float32
BF16 = jnp.bfloat16


def layer_kernel(
    n_sp,
    n_tp,
    lanes,
    tok_ref,
    gain_ref,
    wq_ref,
    wk_ref,
    wv_ref,
    off_ref,
    wout_ref,
    out_ref,
    tok_buf,
    w_buf,
    wo_buf,
    normed,
    kv_out,
    q_out,
    kv_buf,
    q_buf,
    att_out,
    att_buf,
    chain_sem,
    pair_sem,
    load_sem,
    tok_send,
    tok_recv,
    wo_send,
    wo_recv,
    wo_swap,
    kv_send,
    kv_recv,
    q_send,
    q_recv,
    att_send,
    att_recv,
):
    s = lax.axis_index("sp")
    t = lax.axis_index("tp")
    heads = kv_out.shape[0]
    rows = kv_out.shape[1]
    piece = tok_buf.shape[1]
    width = 2 * HEAD_DIM
    groups = n_sp // heads
    a = s // heads
    b = s % heads
    pair_hi = t // lanes
    pair_lo = t % lanes
    n_hi = n_tp // lanes

    loads = [
        pltpu.make_async_copy(tok_ref, tok_buf.at[t], load_sem.at[0]),
        pltpu.make_async_copy(wq_ref, w_buf.at[:, pl.ds(0, width)], load_sem.at[1]),
        pltpu.make_async_copy(wk_ref, w_buf.at[:, pl.ds(width, width)], load_sem.at[2]),
        pltpu.make_async_copy(wv_ref, w_buf.at[:, pl.ds(2 * width, width)], load_sem.at[3]),
        pltpu.make_async_copy(wout_ref, wo_buf.at[t], load_sem.at[4]),
    ]
    for load in loads:
        load.start()

    barrier = pltpu.get_barrier_semaphore()
    for i in range(1, n_tp):
        pl.semaphore_signal(barrier, inc=1, device_id=(s, (t + i) % n_tp), device_id_type=MESH)
    for j in range(1, heads):
        pl.semaphore_signal(barrier, inc=1, device_id=(a * heads + (b + j) % heads, t), device_id_type=MESH)
    has_next = a < groups - 1
    has_prev = a > 0

    @pl.when(has_next)
    def _():
        pl.semaphore_signal(barrier, inc=1, device_id=(s + heads, t), device_id_type=MESH)

    @pl.when(has_prev)
    def _():
        pl.semaphore_signal(barrier, inc=1, device_id=(s - heads, t), device_id_type=MESH)

    along = jnp.minimum(a, 1) + jnp.minimum(groups - 1 - a, 1)
    pl.semaphore_wait(barrier, n_tp - 1 + heads - 1 + along)

    def send(src, dst, send_sem, recv_sem, device):
        return pltpu.make_async_remote_copy(
            src_ref=src,
            dst_ref=dst,
            send_sem=send_sem,
            recv_sem=recv_sem,
            device_id=device,
            device_id_type=MESH,
        )

    def gather(buf, send_sems, recv_sems):
        sends = []
        for i in range(1, n_hi):
            dest = (pair_hi + i) % n_hi * lanes + pair_lo
            sends.append(send(buf.at[t], buf.at[t], send_sems.at[i * lanes], recv_sems.at[t], (s, dest)))
        for j in range(1, lanes):
            dest = pair_hi * lanes + (pair_lo + j) % lanes
            sends.append(send(buf.at[t], buf.at[t], send_sems.at[j], recv_sems.at[t], (s, dest)))
        return sends

    def arrival(buf, recv_sems, source):
        pltpu.make_async_copy(buf.at[source], buf.at[source], recv_sems.at[source]).wait()

    def relays(buf, send_sems, recv_sems, i, source):
        out = []
        for j in range(1, lanes):
            dest = pair_hi * lanes + (pair_lo + j) % lanes
            out.append(
                send(buf.at[source], buf.at[source], send_sems.at[i * lanes + j], recv_sems.at[source], (s, dest))
            )
        return out

    pieces = wo_send.shape[0]
    wo_rows = wo_buf.shape[1] // pieces

    def wo_at(source, c):
        return wo_buf.at[source, pl.ds(pl.multiple_of(c * wo_rows, wo_rows), wo_rows)]

    def start_all(copies):
        for copy in copies:
            copy.start()
            wo_pending.append(copy)

    def wo_send_to(source, c, slot, device):
        return send(wo_at(source, c), wo_at(source, c), wo_send.at[c, slot], wo_recv.at[source, c], device)

    def wo_far(c):
        return [wo_send_to(t, c, i * lanes, (s, (pair_hi + i) % n_hi * lanes + pair_lo)) for i in range(1, n_hi)]

    def wo_near(c, i=0):
        source = (pair_hi + i) % n_hi * lanes + pair_lo
        return [
            wo_send_to(source, c, i * lanes + j, (s, pair_hi * lanes + (pair_lo + j) % lanes))
            for j in range(1, lanes)
        ]

    def wo_wait(source, c):
        pltpu.make_async_copy(wo_at(source, c), wo_at(source, c), wo_recv.at[source, c]).wait()

    def wo_relay(c, across):
        for i in range(1, n_hi):
            source = (pair_hi + i) % n_hi * lanes + pair_lo
            wo_wait(source, c)
            if across:
                for j in range(1, heads):
                    device = (a * heads + (b + j) % heads, t)
                    start_all(
                        [send(wo_at(source, c), wo_at(source, c), wo_swap.at[i, j], wo_recv.at[source, c], device)]
                    )
            start_all(wo_near(c, i))

    def wo_arrival(source):
        for c in range(pieces):
            wo_wait(source, c)

    gain = gain_ref[...]

    def norm(source):
        x = tok_buf[source].astype(F32)
        inv = lax.rsqrt(jnp.mean(x * x, axis=1, keepdims=True) + RMS_EPS)
        normed[pl.ds(pl.multiple_of(source * piece, piece), piece), :] = (x * inv * gain).astype(BF16)

    loads[0].wait()
    pending = gather(tok_buf, tok_send, tok_recv)
    for copy in pending:
        copy.start()

    loads[4].wait()
    wo_pending = []
    for c in [b] + list(range(heads, pieces)):
        start_all(wo_far(c))
    for c in range(pieces):
        start_all(wo_near(c))

    @pl.when(has_next)
    def _():
        pl.semaphore_wait(chain_sem, 1)

    @pl.when(has_prev)
    def _():
        pl.semaphore_signal(chain_sem, inc=1, device_id=(s - heads, t), device_id_type=MESH)

    for j in range(1, heads):
        pl.semaphore_signal(pair_sem, inc=1, device_id=(a * heads + (b + j) % heads, t), device_id_type=MESH)
    norm(t)
    for j in range(1, lanes):
        source = pair_hi * lanes + (pair_lo + j) % lanes
        arrival(tok_buf, tok_recv, source)
        norm(source)
    for i in range(1, n_hi):
        source = (pair_hi + i) % n_hi * lanes + pair_lo
        arrival(tok_buf, tok_recv, source)
        for copy in relays(tok_buf, tok_send, tok_recv, i, source):
            copy.start()
            pending.append(copy)
        norm(source)
    pl.semaphore_wait(pair_sem, heads - 1)
    for i in range(1, n_hi):
        for j in range(1, lanes):
            source = (pair_hi + i) % n_hi * lanes + (pair_lo + j) % lanes
            arrival(tok_buf, tok_recv, source)
            norm(source)
    for load in loads[1:4]:
        load.wait()

    projected = jnp.dot(normed[...], w_buf[...], preferred_element_type=F32).astype(BF16)
    blank = jnp.zeros((rows, HEAD_DIM), BF16)
    for h in range(heads):
        cols = slice(h * HEAD_DIM, (h + 1) * HEAD_DIM)
        keys = projected[:, width:][:, cols]
        vals = projected[:, 2 * width :][:, cols]
        kv_out[h] = jnp.concatenate([keys, vals], axis=1)
        q_out[h] = jnp.concatenate([projected[:, cols] * jnp.asarray(HEAD_DIM**-0.5, BF16), blank], axis=1)

    mine = pl.ds(pl.multiple_of(b * rows, rows), rows)
    kv_sends = []
    for j in range(1, heads):
        h = (b + j) % heads
        dest = (a * heads + h, t)
        kv_sends.append(send(q_out.at[h], q_buf.at[mine], q_send.at[j], q_recv.at[b], dest))
        kv_sends.append(send(kv_out.at[h], kv_buf.at[a, mine], kv_send.at[0, j], kv_recv.at[s], dest))
    for copy in kv_sends:
        copy.start()

    def kv_copy(k, j):
        h = (b + j) % heads
        return send(kv_out.at[h], kv_buf.at[a, mine], kv_send.at[k, j], kv_recv.at[s], ((a + k) * heads + h, t))

    later = groups - 1 - a

    def kv_start(i, carry):
        for j in range(heads):
            kv_copy(i + 1, j).start()
        return carry

    lax.fori_loop(0, later, kv_start, 0)
    wo_relay(b, True)
    kv_buf[a, mine, :] = kv_out[b]
    q_buf[mine, :] = q_out[b]

    for j in range(1, heads):
        peer = (b + j) % heads
        spot = pl.ds(pl.multiple_of(peer * rows, rows), rows)
        pltpu.make_async_copy(q_buf.at[spot], q_buf.at[spot], q_recv.at[peer]).wait()

    span = heads * rows
    offset = off_ref[b]
    row_id = lax.broadcasted_iota(jnp.int32, (span, span), 0)
    col_id = lax.broadcasted_iota(jnp.int32, (span, span), 1)
    below = row_id > col_id
    tri = jnp.where(below, 1.0, 0.0).astype(BF16)
    queries = q_buf[...]

    def block(group, masked, total, kept):
        kv = kv_buf[group]
        z = lax.dot_general(queries, kv, (((1,), (1,)), ((), ())), preferred_element_type=F32) + offset
        log_keep = -(jnp.maximum(z, 0.0) + jnp.log1p(jnp.exp(-jnp.abs(z))))
        log_take = z + log_keep
        if masked:
            log_keep = jnp.where(below, log_keep, 0.0)
        high = log_keep.astype(BF16)
        low = (log_keep - high.astype(F32)).astype(BF16)
        suffix = jnp.dot(high, tri, preferred_element_type=F32) + jnp.dot(low, tri, preferred_element_type=F32)
        weights = jnp.exp(log_take + suffix + kept)
        if masked:
            weights = jnp.where(below, weights, 0.0)
        total = total + jnp.dot(weights.astype(BF16), kv, preferred_element_type=F32)
        return total, kept + suffix[:, :1] + log_keep[:, :1]

    def kv_arrival(group, peer):
        spot = kv_buf.at[group, pl.ds(pl.multiple_of(peer * rows, rows), rows)]
        pltpu.make_async_copy(spot, spot, kv_recv.at[group * heads + peer]).wait()

    for j in range(1, heads):
        kv_arrival(a, (b + j) % heads)
    total, kept = block(a, True, jnp.zeros((span, width), F32), jnp.zeros((span, 1), F32))

    wo_relay(heads, False)

    def absorb(i, carry):
        group = a - 1 - i
        for peer in range(heads):
            kv_arrival(group, peer)
        return block(group, False, *carry)

    total, kept = lax.fori_loop(0, a, absorb, (total, kept))

    att_out[...] = total.astype(BF16).reshape(att_out.shape)
    att_sends = []
    for j in range(heads):
        for i in range(n_tp):
            if i == 0 and j == 0:
                continue
            peer = (b + j) % heads
            other = (t + i) % n_tp
            att_sends.append(
                send(
                    att_out.at[peer * n_tp + other],
                    att_buf.at[t * heads + b],
                    att_send.at[j * n_tp + i],
                    att_recv.at[t * heads + b],
                    (a * heads + peer, other),
                )
            )
    for copy in att_sends:
        copy.start()
    att_buf[t * heads + b] = att_out[b * n_tp + t]

    for c in range(heads + 1, pieces):
        wo_relay(c, False)
    for j in range(1, heads):
        wo_relay((b + j) % heads, False)

    def partial(source):
        for h in range(heads):
            if source is t:
                continue
            arrival(att_buf, att_recv, source * heads + h)
        parts = [att_buf[source * heads + h][:, HEAD_DIM:] for h in range(heads)]
        part = jnp.dot(jnp.concatenate(parts, axis=1), wo_buf[source], preferred_element_type=F32)
        return part.astype(BF16).astype(F32)

    for j in range(1, heads):
        arrival(att_buf, att_recv, t * heads + (b + j) % heads)
    mixed = partial(t)
    for j in range(1, lanes):
        source = pair_hi * lanes + (pair_lo + j) % lanes
        wo_arrival(source)
        mixed = mixed + partial(source)
    for i in range(1, n_hi):
        mixed = mixed + partial((pair_hi + i) % n_hi * lanes + pair_lo)
    for i in range(1, n_hi):
        for j in range(1, lanes):
            source = (pair_hi + i) % n_hi * lanes + (pair_lo + j) % lanes
            wo_arrival(source)
            mixed = mixed + partial(source)
    out_ref[...] = mixed.astype(BF16)

    for copy in pending + wo_pending + kv_sends + att_sends:
        copy.wait_send()

    def kv_done(i, carry):
        for j in range(heads):
            kv_copy(i + 1, j).wait_send()
        return carry

    lax.fori_loop(0, later, kv_done, 0)


def per_device(tokens, norm_gain, w_query, w_key, w_value, score_offset, w_out):
    n_tp = lax.axis_size("tp")
    n_sp = lax.axis_size("sp")
    piece, model = tokens.shape
    width = w_query.shape[1]
    heads = score_offset.shape[0]
    rows = piece * n_tp
    lanes = 2 if n_tp % 2 == 0 else 1
    groups = n_sp // heads
    lane_width = 2 * HEAD_DIM
    dma = pltpu.SemaphoreType.DMA
    anywhere = pl.BlockSpec(memory_space=pl.ANY)
    vmem = pl.BlockSpec(memory_space=pltpu.VMEM)
    return pl.pallas_call(
        functools.partial(layer_kernel, n_sp, n_tp, lanes),
        out_shape=pltpu.VMEM((piece, w_out.shape[1]), BF16),
        in_specs=[
            anywhere,
            vmem,
            anywhere,
            anywhere,
            anywhere,
            pl.BlockSpec(memory_space=pltpu.SMEM),
            anywhere,
        ],
        out_specs=vmem,
        scratch_shapes=[
            pltpu.VMEM((n_tp, piece, model), BF16),
            pltpu.VMEM((model, 3 * width), BF16),
            pltpu.VMEM((n_tp, width, w_out.shape[1]), BF16),
            pltpu.VMEM((rows, model), BF16),
            pltpu.VMEM((heads, rows, lane_width), BF16),
            pltpu.VMEM((heads, rows, lane_width), BF16),
            pltpu.VMEM((groups, heads * rows, lane_width), BF16),
            pltpu.VMEM((heads * rows, lane_width), BF16),
            pltpu.VMEM((heads * n_tp, piece, lane_width), BF16),
            pltpu.VMEM((heads * n_tp, piece, lane_width), BF16),
            pltpu.SemaphoreType.REGULAR,
            pltpu.SemaphoreType.REGULAR,
            dma((5,)),
            dma((n_tp,)),
            dma((n_tp,)),
            dma((2 * heads, n_tp)),
            dma((n_tp, 2 * heads)),
            dma((n_tp // lanes, heads)),
            dma((groups, heads)),
            dma((n_sp,)),
            dma((heads,)),
            dma((heads,)),
            dma((heads * n_tp,)),
            dma((heads * n_tp,)),
        ],
        compiler_params=pltpu.CompilerParams(collective_id=0, has_side_effects=True),
    )(tokens, norm_gain.reshape(1, model), w_query, w_key, w_value, score_offset, w_out)


def solution(mesh):
    return jax.shard_map(
        per_device,
        mesh=mesh,
        in_specs=(
            P(("sp", "tp"), None),
            P(),
            P(None, "tp"),
            P(None, "tp"),
            P(None, "tp"),
            P("tp"),
            P("tp", None),
        ),
        out_specs=P(("sp", "tp"), None),
        check_vma=False,
    )
```

```python
import functools

import jax
import jax.numpy as jnp
from jax import lax
from jax.experimental import pallas as pl
from jax.experimental.pallas import tpu as pltpu
from jax.sharding import PartitionSpec as P

HEAD_DIM = 64
RMS_EPS = 1e-06
MESH = pl.DeviceIdType.MESH
F32 = jnp.float32
BF16 = jnp.bfloat16


def layer_kernel(
    n_sp,
    n_tp,
    lanes,
    tok_ref,
    gain_ref,
    wq_ref,
    wk_ref,
    wv_ref,
    off_ref,
    wout_ref,
    out_ref,
    tok_buf,
    w_buf,
    wo_buf,
    normed,
    kv_out,
    q_out,
    kv_buf,
    q_buf,
    att_out,
    att_buf,
    chain_sem,
    pair_sem,
    load_sem,
    tok_send,
    tok_recv,
    wo_send,
    wo_recv,
    wo_swap,
    kv_send,
    kv_recv,
    q_send,
    q_recv,
    att_send,
    att_recv,
):
    s = lax.axis_index("sp")
    t = lax.axis_index("tp")
    heads = kv_out.shape[0]
    rows = kv_out.shape[1]
    piece = tok_buf.shape[1]
    width = 2 * HEAD_DIM
    groups = n_sp // heads
    a = s // heads
    b = s % heads
    pair_hi = t // lanes
    pair_lo = t % lanes
    n_hi = n_tp // lanes

    loads = [
        pltpu.make_async_copy(tok_ref, tok_buf.at[t], load_sem.at[0]),
        pltpu.make_async_copy(wq_ref, w_buf.at[:, pl.ds(0, width)], load_sem.at[1]),
        pltpu.make_async_copy(wk_ref, w_buf.at[:, pl.ds(width, width)], load_sem.at[2]),
        pltpu.make_async_copy(wv_ref, w_buf.at[:, pl.ds(2 * width, width)], load_sem.at[3]),
        pltpu.make_async_copy(wout_ref, wo_buf.at[t], load_sem.at[4]),
    ]
    for load in loads:
        load.start()

    barrier = pltpu.get_barrier_semaphore()
    for i in range(1, n_tp):
        pl.semaphore_signal(barrier, inc=1, device_id=(s, (t + i) % n_tp), device_id_type=MESH)
    for j in range(1, heads):
        pl.semaphore_signal(barrier, inc=1, device_id=(a * heads + (b + j) % heads, t), device_id_type=MESH)
    has_next = a < groups - 1
    has_prev = a > 0

    @pl.when(has_next)
    def _():
        pl.semaphore_signal(barrier, inc=1, device_id=(s + heads, t), device_id_type=MESH)

    @pl.when(has_prev)
    def _():
        pl.semaphore_signal(barrier, inc=1, device_id=(s - heads, t), device_id_type=MESH)

    along = jnp.minimum(a, 1) + jnp.minimum(groups - 1 - a, 1)
    pl.semaphore_wait(barrier, n_tp - 1 + heads - 1 + along)

    def send(src, dst, send_sem, recv_sem, device):
        return pltpu.make_async_remote_copy(
            src_ref=src,
            dst_ref=dst,
            send_sem=send_sem,
            recv_sem=recv_sem,
            device_id=device,
            device_id_type=MESH,
        )

    def gather(buf, send_sems, recv_sems):
        sends = []
        for i in range(1, n_hi):
            dest = (pair_hi + i) % n_hi * lanes + pair_lo
            sends.append(send(buf.at[t], buf.at[t], send_sems.at[i * lanes], recv_sems.at[t], (s, dest)))
        for j in range(1, lanes):
            dest = pair_hi * lanes + (pair_lo + j) % lanes
            sends.append(send(buf.at[t], buf.at[t], send_sems.at[j], recv_sems.at[t], (s, dest)))
        return sends

    def arrival(buf, recv_sems, source):
        pltpu.make_async_copy(buf.at[source], buf.at[source], recv_sems.at[source]).wait()

    def relays(buf, send_sems, recv_sems, i, source):
        out = []
        for j in range(1, lanes):
            dest = pair_hi * lanes + (pair_lo + j) % lanes
            out.append(
                send(buf.at[source], buf.at[source], send_sems.at[i * lanes + j], recv_sems.at[source], (s, dest))
            )
        return out

    pieces = wo_send.shape[0]
    wo_rows = wo_buf.shape[1] // pieces

    def wo_at(source, c):
        return wo_buf.at[source, pl.ds(pl.multiple_of(c * wo_rows, wo_rows), wo_rows)]

    def start_all(copies):
        for copy in copies:
            copy.start()
            wo_pending.append(copy)

    def wo_send_to(source, c, slot, device):
        return send(wo_at(source, c), wo_at(source, c), wo_send.at[c, slot], wo_recv.at[source, c], device)

    def wo_far(c):
        return [wo_send_to(t, c, i * lanes, (s, (pair_hi + i) % n_hi * lanes + pair_lo)) for i in range(1, n_hi)]

    def wo_near(c, i=0):
        source = (pair_hi + i) % n_hi * lanes + pair_lo
        return [
            wo_send_to(source, c, i * lanes + j, (s, pair_hi * lanes + (pair_lo + j) % lanes))
            for j in range(1, lanes)
        ]

    def wo_wait(source, c):
        pltpu.make_async_copy(wo_at(source, c), wo_at(source, c), wo_recv.at[source, c]).wait()

    def wo_relay(c, across):
        for i in range(1, n_hi):
            source = (pair_hi + i) % n_hi * lanes + pair_lo
            wo_wait(source, c)
            if across:
                for j in range(1, heads):
                    device = (a * heads + (b + j) % heads, t)
                    start_all(
                        [send(wo_at(source, c), wo_at(source, c), wo_swap.at[i, j], wo_recv.at[source, c], device)]
                    )
            start_all(wo_near(c, i))

    def wo_arrival(source):
        for c in range(pieces):
            wo_wait(source, c)

    gain = gain_ref[...]

    def norm(source):
        x = tok_buf[source].astype(F32)
        inv = lax.rsqrt(jnp.mean(x * x, axis=1, keepdims=True) + RMS_EPS)
        normed[pl.ds(pl.multiple_of(source * piece, piece), piece), :] = (x * inv * gain).astype(BF16)

    loads[0].wait()
    pending = gather(tok_buf, tok_send, tok_recv)
    for copy in pending:
        copy.start()

    loads[4].wait()
    wo_pending = []
    for c in [b] + list(range(heads, pieces)):
        start_all(wo_far(c))
    for c in range(pieces):
        start_all(wo_near(c))

    @pl.when(has_next)
    def _():
        pl.semaphore_wait(chain_sem, 1)

    @pl.when(has_prev)
    def _():
        pl.semaphore_signal(chain_sem, inc=1, device_id=(s - heads, t), device_id_type=MESH)

    for j in range(1, heads):
        pl.semaphore_signal(pair_sem, inc=1, device_id=(a * heads + (b + j) % heads, t), device_id_type=MESH)
    norm(t)
    for j in range(1, lanes):
        source = pair_hi * lanes + (pair_lo + j) % lanes
        arrival(tok_buf, tok_recv, source)
        norm(source)
    for load in loads[1:4]:
        load.wait()

    chunk = lanes * piece
    later = groups - 1 - a
    kv_sends = []

    def project(i):
        span = pl.ds(pl.multiple_of((pair_hi + i) % n_hi * chunk, chunk), chunk)
        projected = jnp.dot(normed[span, :], w_buf[...], preferred_element_type=F32).astype(BF16)
        blank = jnp.zeros((chunk, HEAD_DIM), BF16)
        for h in range(heads):
            cols = slice(h * HEAD_DIM, (h + 1) * HEAD_DIM)
            keys = projected[:, width:][:, cols]
            vals = projected[:, 2 * width :][:, cols]
            kv_out[h, span, :] = jnp.concatenate([keys, vals], axis=1)
            q_out[h, span, :] = jnp.concatenate([projected[:, cols] * jnp.asarray(HEAD_DIM**-0.5, BF16), blank], axis=1)

    def spans(i):
        part = (pair_hi + i) % n_hi
        here = pl.ds(pl.multiple_of(part * chunk, chunk), chunk)
        there = pl.ds(pl.multiple_of(b * rows + part * chunk, chunk), chunk)
        return part, here, there

    def kv_copy(k, j, i):
        h = (b + j) % heads
        part, here, there = spans(i)
        return send(
            kv_out.at[h, here],
            kv_buf.at[a, there],
            kv_send.at[k, i * heads + j],
            kv_recv.at[s, part],
            ((a + k) * heads + h, t),
        )

    def send_chunks(i):
        for j in range(1, heads):
            h = (b + j) % heads
            part, here, there = spans(i)
            pair = [
                send(q_out.at[h, here], q_buf.at[there], q_send.at[j, i], q_recv.at[b, part], (a * heads + h, t)),
                kv_copy(0, j, i),
            ]
            for copy in pair:
                copy.start()
            kv_sends.extend(pair)

        def kv_start(k, carry):
            for j in range(heads):
                kv_copy(k, j, i).start()
            return carry

        lax.fori_loop(1, later + 1, kv_start, 0)

    project(0)
    pl.semaphore_wait(pair_sem, heads - 1)
    send_chunks(0)
    for i in range(1, n_hi):
        source = (pair_hi + i) % n_hi * lanes + pair_lo
        arrival(tok_buf, tok_recv, source)
        for copy in relays(tok_buf, tok_send, tok_recv, i, source):
            copy.start()
            pending.append(copy)
        norm(source)
    for i in range(1, n_hi):
        for j in range(1, lanes):
            source = (pair_hi + i) % n_hi * lanes + (pair_lo + j) % lanes
            arrival(tok_buf, tok_recv, source)
            norm(source)
    for i in range(1, n_hi):
        project(i)
        send_chunks(i)
    mine = pl.ds(pl.multiple_of(b * rows, rows), rows)
    wo_relay(b, True)
    kv_buf[a, mine, :] = kv_out[b]
    q_buf[mine, :] = q_out[b]

    for j in range(1, heads):
        peer = (b + j) % heads
        for part in range(n_hi):
            spot = pl.ds(pl.multiple_of(peer * rows + part * chunk, chunk), chunk)
            pltpu.make_async_copy(q_buf.at[spot], q_buf.at[spot], q_recv.at[peer, part]).wait()

    span = heads * rows
    offset = off_ref[b]
    row_id = lax.broadcasted_iota(jnp.int32, (span, span), 0)
    col_id = lax.broadcasted_iota(jnp.int32, (span, span), 1)
    below = row_id > col_id
    tri = jnp.where(below, 1.0, 0.0).astype(BF16)
    queries = q_buf[...]

    def block(group, masked, total, kept):
        kv = kv_buf[group]
        z = lax.dot_general(queries, kv, (((1,), (1,)), ((), ())), preferred_element_type=F32) + offset
        log_keep = -(jnp.maximum(z, 0.0) + jnp.log1p(jnp.exp(-jnp.abs(z))))
        log_take = z + log_keep
        if masked:
            log_keep = jnp.where(below, log_keep, 0.0)
        high = log_keep.astype(BF16)
        low = (log_keep - high.astype(F32)).astype(BF16)
        suffix = jnp.dot(high, tri, preferred_element_type=F32) + jnp.dot(low, tri, preferred_element_type=F32)
        weights = jnp.exp(log_take + suffix + kept)
        if masked:
            weights = jnp.where(below, weights, 0.0)
        total = total + jnp.dot(weights.astype(BF16), kv, preferred_element_type=F32)
        return total, kept + suffix[:, :1] + log_keep[:, :1]

    def kv_arrival(group, peer):
        for part in range(n_hi):
            spot = kv_buf.at[group, pl.ds(pl.multiple_of(peer * rows + part * chunk, chunk), chunk)]
            pltpu.make_async_copy(spot, spot, kv_recv.at[group * heads + peer, part]).wait()

    for j in range(1, heads):
        kv_arrival(a, (b + j) % heads)
    total, kept = block(a, True, jnp.zeros((span, width), F32), jnp.zeros((span, 1), F32))

    wo_relay(heads, False)

    def absorb(i, carry):
        group = a - 1 - i
        for peer in range(heads):
            kv_arrival(group, peer)
        return block(group, False, *carry)

    total, kept = lax.fori_loop(0, a, absorb, (total, kept))

    att_out[...] = total.astype(BF16).reshape(att_out.shape)
    att_sends = []
    for j in range(heads):
        for i in range(n_tp):
            if i == 0 and j == 0:
                continue
            peer = (b + j) % heads
            other = (t + i) % n_tp
            att_sends.append(
                send(
                    att_out.at[peer * n_tp + other],
                    att_buf.at[t * heads + b],
                    att_send.at[j * n_tp + i],
                    att_recv.at[t * heads + b],
                    (a * heads + peer, other),
                )
            )
    for copy in att_sends:
        copy.start()
    att_buf[t * heads + b] = att_out[b * n_tp + t]

    for c in range(heads + 1, pieces):
        wo_relay(c, False)
    for j in range(1, heads):
        wo_relay((b + j) % heads, False)

    def partial(source):
        for h in range(heads):
            if source is t:
                continue
            arrival(att_buf, att_recv, source * heads + h)
        parts = [att_buf[source * heads + h][:, HEAD_DIM:] for h in range(heads)]
        part = jnp.dot(jnp.concatenate(parts, axis=1), wo_buf[source], preferred_element_type=F32)
        return part.astype(BF16).astype(F32)

    for j in range(1, heads):
        arrival(att_buf, att_recv, t * heads + (b + j) % heads)
    mixed = partial(t)
    for j in range(1, lanes):
        source = pair_hi * lanes + (pair_lo + j) % lanes
        wo_arrival(source)
        mixed = mixed + partial(source)
    for i in range(1, n_hi):
        mixed = mixed + partial((pair_hi + i) % n_hi * lanes + pair_lo)
    for i in range(1, n_hi):
        for j in range(1, lanes):
            source = (pair_hi + i) % n_hi * lanes + (pair_lo + j) % lanes
            wo_arrival(source)
            mixed = mixed + partial(source)
    out_ref[...] = mixed.astype(BF16)

    for copy in pending + wo_pending + kv_sends + att_sends:
        copy.wait_send()

    def kv_done(k, carry):
        for j in range(heads):
            for i in range(n_hi):
                kv_copy(k, j, i).wait_send()
        return carry

    lax.fori_loop(1, later + 1, kv_done, 0)


def per_device(tokens, norm_gain, w_query, w_key, w_value, score_offset, w_out):
    n_tp = lax.axis_size("tp")
    n_sp = lax.axis_size("sp")
    piece, model = tokens.shape
    width = w_query.shape[1]
    heads = score_offset.shape[0]
    rows = piece * n_tp
    lanes = 2 if n_tp % 2 == 0 else 1
    groups = n_sp // heads
    lane_width = 2 * HEAD_DIM
    dma = pltpu.SemaphoreType.DMA
    anywhere = pl.BlockSpec(memory_space=pl.ANY)
    vmem = pl.BlockSpec(memory_space=pltpu.VMEM)
    return pl.pallas_call(
        functools.partial(layer_kernel, n_sp, n_tp, lanes),
        out_shape=pltpu.VMEM((piece, w_out.shape[1]), BF16),
        in_specs=[
            anywhere,
            vmem,
            anywhere,
            anywhere,
            anywhere,
            pl.BlockSpec(memory_space=pltpu.SMEM),
            anywhere,
        ],
        out_specs=vmem,
        scratch_shapes=[
            pltpu.VMEM((n_tp, piece, model), BF16),
            pltpu.VMEM((model, 3 * width), BF16),
            pltpu.VMEM((n_tp, width, w_out.shape[1]), BF16),
            pltpu.VMEM((rows, model), BF16),
            pltpu.VMEM((heads, rows, lane_width), BF16),
            pltpu.VMEM((heads, rows, lane_width), BF16),
            pltpu.VMEM((groups, heads * rows, lane_width), BF16),
            pltpu.VMEM((heads * rows, lane_width), BF16),
            pltpu.VMEM((heads * n_tp, piece, lane_width), BF16),
            pltpu.VMEM((heads * n_tp, piece, lane_width), BF16),
            pltpu.SemaphoreType.REGULAR,
            pltpu.SemaphoreType.REGULAR,
            dma((5,)),
            dma((n_tp,)),
            dma((n_tp,)),
            dma((2 * heads, n_tp)),
            dma((n_tp, 2 * heads)),
            dma((n_tp // lanes, heads)),
            dma((groups, heads * (n_tp // lanes))),
            dma((n_sp, n_tp // lanes)),
            dma((heads, n_tp // lanes)),
            dma((heads, n_tp // lanes)),
            dma((heads * n_tp,)),
            dma((heads * n_tp,)),
        ],
        compiler_params=pltpu.CompilerParams(collective_id=0, has_side_effects=True),
    )(tokens, norm_gain.reshape(1, model), w_query, w_key, w_value, score_offset, w_out)


def solution(mesh):
    return jax.shard_map(
        per_device,
        mesh=mesh,
        in_specs=(
            P(("sp", "tp"), None),
            P(),
            P(None, "tp"),
            P(None, "tp"),
            P(None, "tp"),
            P("tp"),
            P("tp", None),
        ),
        out_specs=P(("sp", "tp"), None),
        check_vma=False,
    )
```
